128 devices in a mesh: ep: 16 (over z, x), tp: 8 (over y, core).
Axes of the slice: x: 4, y: 4, z: 4, core: 2. Of those that a mesh axis runs over, the one named last changes fastest.
Arguments:
- mixer_rows: bfloat16 [4096, 4096], P('ep'), may hold values from -8 to 8, as said below
- mixer_gain: float32 [4096], replicated, may hold values from 0.1 to 1.9
- gate_proj: bfloat16 [4096, 4096], P(None, 'tp'), may hold values from -0.09375 to 0.09375
- input_proj: bfloat16 [4096, 4096], P(None, 'tp'), may hold values from -0.09375 to 0.09375
- conv_taps: float32 [4, 4096], P(None, 'tp'), may hold values from -2 to 2
- input_gates: bfloat16 [16, 256, 256], P('tp'), may hold values from -0.375 to 0.375
- decay_gates: bfloat16 [16, 256, 256], P('tp'), may hold values from -0.375 to 0.375
- decay_offset: float32 [4096], P('tp'), may hold values from 4.8 to 13, as said below
- out_proj: bfloat16 [4096, 4096], P('tp'), may hold values from -0.09375 to 0.09375
- mixer_scale: float32 [4096], replicated, may hold values from 0.1 to 1.9
- expert_rows: bfloat16 [4096, 4096], P('ep'), may hold values from -6 to 6
- expert_gain: float32 [4096], replicated, may hold values from 0.1 to 1.9
- route_ids: int32 [4096, 2], P('ep'), may hold values from 0 to 15, all different within a row; in each aligned block of 256 rows (0 to 255, 256 to 511, ...) at most 48 rows name the same one
- route_weights: float32 [4096, 2], P('ep'), may hold values from 0.5 to 2
- expert_gate: bfloat16 [16, 4096, 1024], P('ep', None, 'tp'), may hold values from -0.09375 to 0.09375
- expert_up: bfloat16 [16, 4096, 1024], P('ep', None, 'tp'), may hold values from -0.09375 to 0.09375
- expert_down: bfloat16 [16, 1024, 4096], P('ep', 'tp'), may hold values from -0.1875 to 0.1875
- shared_gate: bfloat16 [4096, 1024], P(None, 'tp'), may hold values from -0.09375 to 0.09375
- shared_up: bfloat16 [4096, 1024], P(None, 'tp'), may hold values from -0.09375 to 0.09375
- shared_down: bfloat16 [1024, 4096], P('tp'), may hold values from -0.1875 to 0.1875
- expert_scale: float32 [4096], replicated, may hold values from 0.1 to 1.9
Outputs:
- mixer_out: bfloat16 [4096, 4096], P(('ep', 'tp'))
- expert_out: bfloat16 [4096, 4096], P(('ep', 'tp'))
The draws below stay inside these ranges and needn't reach their ends.
Inputs may be any that keep to these rules, and one draw needn't show every extreme that they name: `mixer_rows`: order one, with a common direction whose weight drifts slowly along the sequence. `decay_offset`: the even channels forget within some 30 to 200 tokens; the odd channels keep 5 to 90 percent of their state over the whole sequence of 4096 tokens. `route_ids`: each row names 2 different experts; within the rows of one index of ep (aligned blocks of 256 rows) no expert is named by more than 48 rows, and in some blocks one is named by exactly 48.
All inputs are finite; a program needn't handle non-finite values.
Results may differ from the reference program's by a relative error of at most 0.0033.
The reference program's roundings to bfloat16 on the way count: a program that leaves them out, or rounds other values in their place, can miss the bound.
Values may be sent and summed in bfloat16 or wider, within the bound.
No kernel may reach another device: no remote copies, remote signals or barrier semaphores. Data moves between devices by JAX's collectives and lax.ppermute only.
A program may use at most 192 MiB of HBM per device.

```python
import math
import jax
import jax.numpy as jnp
import numpy as np
from jax import lax

D = 4096
RNN_BLOCKS = 16
BLOCK_WIDTH = 256
CONV = 4
EXPERT_HIDDEN = 1024
SHARED_HIDDEN = 1024
TOP_K = 2
ROWS = 256
EXPERTS = 16
TOKENS = 4096
CAP = 48
N_EP = 16


def draw_mixer_rows(key, part):
    noise_key, direction_key, phase_key = jax.random.split(key, 3)
    noise_part = jax.random.normal(noise_key, (TOKENS, D), jnp.float32)
    direction = jax.random.normal(direction_key, (D,), jnp.float32)
    phase_shift = jax.random.uniform(phase_key, (), jnp.float32, 0.0, 2.0 * math.pi)
    positions = jnp.arange(TOKENS, dtype=jnp.float32) / TOKENS
    drift_level = 2.0 * jnp.sin(3.0 * math.pi * positions + phase_shift)
    values = noise_part + drift_level[:, None] * direction[None, :]
    return jnp.clip(values, -8.0, 8.0).astype(jnp.bfloat16)


def draw_decay_offset(key, part):
    fast_key, slow_key = jax.random.split(key)
    fast_part = jax.random.uniform(fast_key, (D,), jnp.float32, 4.8, 6.7)
    slow_part = math.log(TOKENS) + jax.random.uniform(slow_key, (D,), jnp.float32, 0.3, 3.6)
    parity = jnp.arange(D) % 2
    return jnp.where(parity == 0, fast_part, slow_part).astype(jnp.float32)


def levels(key, dims, pieces, least, high):
    gain = 1.0
    for axis_at, shards_of in pieces:
        heights = jax.random.uniform(jax.random.fold_in(jax.random.fold_in(key, 6), axis_at), (shards_of,), jnp.float32, least / len(pieces), high / len(pieces))
        gain = gain * jnp.repeat(jnp.exp(heights), dims[axis_at] // shards_of).reshape((-1,) + (1,) * (len(dims) - 1 - axis_at))
    return gain


def routed_block(key, own, number, rows, amount, top, most, skew):
    order = jax.random.permutation(key, amount)
    crowded, common = portions_of(amount, rows * top, most, skew, True), portions_of(amount, rows * top, most, skew, False)
    places = jnp.arange(amount)

    def named(lengths, offset_by):
        used = int((lengths > 0).sum())
        fixed = max(1, used // 4)
        shifted = fixed + (places - fixed + offset_by * (used - fixed)) % max(1, amount - fixed)
        return jnp.zeros((amount,), jnp.int32).at[order[jnp.where(places < fixed, places, shifted)]].set(jnp.asarray(lengths, jnp.int32))

    lengths = jnp.where(number % 4 == 0, named(crowded, number // 4), named(common, number - number // 4 - 1))
    mixed = jax.random.permutation(jax.random.fold_in(own, 3), amount)
    donor, sink = mixed[0:amount // 2 * 2:2], mixed[1:amount // 2 * 2:2]
    room = jnp.minimum(lengths[donor] - 1, most - lengths[sink]) // 2
    room = jnp.where((donor == order[0]) | (sink == order[0]) | (lengths[sink] == 0), 0, jnp.maximum(room, 0))
    shifted = jax.random.randint(jax.random.fold_in(own, 4), (amount // 2,), 0, 1 << 20) % (room + 1)
    lengths = lengths.at[donor].add(-shifted).at[sink].add(shifted)
    members = jnp.searchsorted(jnp.cumsum(lengths), jnp.arange(rows * top), side="right").astype(jnp.int32)
    listing = members.reshape(top, rows).T
    listing = listing[jax.random.permutation(jax.random.fold_in(own, 1), rows)]
    offset_by = jax.random.randint(jax.random.fold_in(own, 2), (rows, 1), 0, top)
    return jnp.take_along_axis(listing, (jnp.arange(top)[None, :] + offset_by) % top, axis=1)


def portions_of(amount, total, bound, slope, full):
    portions = [(1 << 20) // math.isqrt(standing ** slope) + 1 for standing in range(1, amount + 1)]
    largest = bound if full else min(bound, max(-(-total // amount), total * portions[0] // sum(portions)))
    least = 1 if total - largest >= amount - 1 else 0
    counts, spare = [largest] + [least] * (amount - 1), total - largest - least * (amount - 1)
    while spare > 0:
        free = [i for i in range(1, amount) if counts[i] < largest] or [i for i in range(1, amount) if counts[i] < bound]
        whole, budget = sum([portions[i] for i in free]), spare
        for i in free:
            more = min(bound - counts[i], max(1, budget * portions[i] // whole), spare)
            counts[i] = counts[i] + more
            spare = spare - more
    return np.array(counts)


def centred(stream_key, shape, deviation, reach, cuts=(), kind=jnp.bfloat16):
    array = jax.random.normal(stream_key, shape, jnp.float32) * deviation
    if len(cuts) > 0:
        array = levels(stream_key, shape, cuts, -0.22, 0.18) * array
    return jnp.clip(array, min=-reach, max=reach).astype(kind)


def setup_inputs(seed: int = 0) -> dict:
    keys = jax.random.split(jax.random.key(seed), 22)
    mixer_rows = draw_mixer_rows(jax.random.fold_in(keys[21], 71), 0)
    mixer_gain = jnp.clip(1.0 + 0.18 * jax.random.normal(keys[1], (D,), jnp.float32), 0.1, 1.9)
    gate_proj = centred(keys[2], (D, D), D ** -0.5, 0.09375, ((1, 8),))
    input_proj = centred(keys[3], (D, D), D ** -0.5, 0.09375, ((1, 8),))
    conv_taps = centred(keys[4], (CONV, D), 0.5, 2.0, ((1, 8),), jnp.float32)
    input_gates = centred(keys[5], (RNN_BLOCKS, BLOCK_WIDTH, BLOCK_WIDTH), BLOCK_WIDTH ** -0.5, 0.375, ((0, 8),))
    decay_gates = centred(keys[6], (RNN_BLOCKS, BLOCK_WIDTH, BLOCK_WIDTH), BLOCK_WIDTH ** -0.5, 0.375, ((0, 8),))
    decay_offset = draw_decay_offset(jax.random.fold_in(keys[21], 71), 0)
    out_proj = centred(keys[8], (D, D), D ** -0.5, 0.09375, ((0, 8),))
    mixer_scale = jnp.clip(1.0 + 0.18 * jax.random.normal(keys[9], (D,), jnp.float32), 0.1, 1.9)
    expert_rows = centred(keys[10], (TOKENS, D), 1.0, 6.0, ((0, 16),))
    expert_gain = jnp.clip(1.0 + 0.18 * jax.random.normal(keys[11], (D,), jnp.float32), 0.1, 1.9)
    route_ids_keys = jax.random.split(jax.random.fold_in(keys[12], 1), TOKENS // ROWS)
    route_ids_turns = jax.random.permutation(jax.random.fold_in(keys[12], 3), TOKENS // ROWS)
    route_ids = jax.vmap(lambda own, number: routed_block(jax.random.fold_in(keys[12], 2), own, number, ROWS, EXPERTS, TOP_K, CAP, 1))(route_ids_keys, route_ids_turns).reshape((TOKENS, TOP_K))
    route_weights = jnp.clip(0.5 + 1.5 * jax.random.uniform(keys[13], (TOKENS, TOP_K), jnp.float32) ** levels(keys[13], (TOKENS, TOP_K), ((0, 16),), -0.2, 0.2), 0.5, 2.0)
    expert_gate = centred(keys[14], (EXPERTS, D, EXPERT_HIDDEN), D ** -0.5, 0.09375, ((0, 16), (2, 8)))
    expert_up = centred(keys[15], (EXPERTS, D, EXPERT_HIDDEN), D ** -0.5, 0.09375, ((0, 16), (2, 8)))
    expert_down = centred(keys[16], (EXPERTS, EXPERT_HIDDEN, D), EXPERT_HIDDEN ** -0.5, 0.1875, ((0, 16), (1, 8)))
    shared_gate = centred(keys[17], (D, SHARED_HIDDEN), D ** -0.5, 0.09375, ((1, 8),))
    shared_up = centred(keys[18], (D, SHARED_HIDDEN), D ** -0.5, 0.09375, ((1, 8),))
    shared_down = centred(keys[19], (SHARED_HIDDEN, D), SHARED_HIDDEN ** -0.5, 0.1875, ((0, 8),))
    expert_scale = jnp.clip(1.0 + 0.18 * jax.random.normal(keys[20], (D,), jnp.float32), 0.1, 1.9)
    return dict(mixer_rows=mixer_rows, mixer_gain=mixer_gain, gate_proj=gate_proj, input_proj=input_proj, conv_taps=conv_taps, input_gates=input_gates, decay_gates=decay_gates, decay_offset=decay_offset, out_proj=out_proj, mixer_scale=mixer_scale, expert_rows=expert_rows, expert_gain=expert_gain, route_ids=route_ids, route_weights=route_weights, expert_gate=expert_gate, expert_up=expert_up, expert_down=expert_down, shared_gate=shared_gate, shared_up=shared_up, shared_down=shared_down, expert_scale=expert_scale)


eps = 1e-06
lru_power = 8.0

def rms_scale(values, scale):
    floats = values.astype(jnp.float32)
    return floats * lax.rsqrt(lax.optimization_barrier(jnp.mean(floats * floats, axis=-1, keepdims=True)) + eps) * scale

def linear_pair(earlier, later):
    return (earlier[0] * later[0], later[0] * earlier[1] + later[1])

def slot_table(route_ids, expert_count, capacity):
    id_list = route_ids.reshape(-1).astype(jnp.int32)
    indicator = (id_list[:, None] == jnp.arange(expert_count, dtype=jnp.int32)[None, :]).astype(jnp.int32)
    earlier_count = (jnp.cumsum(indicator, axis=0).astype(jnp.int32) - indicator).astype(jnp.int32)
    position = lax.optimization_barrier(jnp.sum(earlier_count * indicator, axis=1)).astype(jnp.int32)
    slot_ids = (id_list * capacity + position).astype(jnp.int32)
    matched = (slot_ids[None, :] == jnp.arange(expert_count * capacity, dtype=jnp.int32)[:, None]).astype(jnp.int32)
    source = lax.optimization_barrier(jnp.sum(matched * jnp.arange(id_list.shape[0], dtype=jnp.int32)[None, :], axis=1)).astype(jnp.int32)
    filled = lax.optimization_barrier(jnp.sum(matched, axis=1)) > 0
    return (slot_ids, source, filled)

def mixer_half(mixer_rows, mixer_gain, gate_proj, input_proj, conv_taps, input_gates, decay_gates, decay_offset, out_proj, mixer_scale):
    row_count = mixer_rows.shape[0]
    normed = rms_scale(mixer_rows, mixer_gain).astype(jnp.bfloat16)
    gate_branch = jax.nn.gelu(jnp.dot(normed, gate_proj, preferred_element_type=jnp.float32))
    branch = jnp.dot(normed, input_proj, preferred_element_type=jnp.float32).astype(jnp.bfloat16)
    tap_count = conv_taps.shape[0]
    padded = jnp.concatenate([jnp.zeros((tap_count - 1, branch.shape[1]), branch.dtype), branch], axis=0)
    conv_sum = conv_taps[0] * padded[0:row_count].astype(jnp.float32)
    for tap_index in range(1, tap_count):
        conv_sum = conv_sum + conv_taps[tap_index] * padded[tap_index:tap_index + row_count].astype(jnp.float32)
    conv_out = conv_sum.astype(jnp.bfloat16)
    block_rows = conv_out.astype(jnp.float32).reshape(row_count, input_gates.shape[0], input_gates.shape[1])
    input_gate = jax.nn.sigmoid(jnp.einsum('rbi,bij->rbj', block_rows, input_gates.astype(jnp.float32))).reshape(row_count, -1)
    decay_gate = jax.nn.sigmoid(jnp.einsum('rbi,bij->rbj', block_rows, decay_gates.astype(jnp.float32))).reshape(row_count, -1)
    log_decay = -lru_power * decay_gate * jax.nn.softplus(-decay_offset)
    positions = jnp.arange(row_count, dtype=jnp.int32)
    input_scale = jnp.where((positions == 0)[:, None], 1.0, jnp.sqrt(-jnp.expm1(2.0 * log_decay)))
    drive_term = input_scale * input_gate * conv_out.astype(jnp.float32)
    decay_product, states = lax.associative_scan(linear_pair, (jnp.exp(log_decay), drive_term), axis=0)
    gated_rows = (gate_branch * states).astype(jnp.bfloat16)
    mixer_sum = jnp.dot(gated_rows, out_proj, preferred_element_type=jnp.float32)
    return rms_scale(mixer_sum, mixer_scale).astype(jnp.bfloat16)

def expert_half(expert_rows, expert_gain, route_ids, route_weights, expert_gate, expert_up, expert_down, shared_gate, shared_up, shared_down, expert_scale):
    expert_normed = rms_scale(expert_rows, expert_gain).astype(jnp.bfloat16)
    expert_count = expert_gate.shape[0]
    top_count = route_ids.shape[1]
    row_width = expert_rows.shape[1]
    gate_whole = expert_gate.astype(jnp.float32)
    up_whole = expert_up.astype(jnp.float32)
    down_whole = expert_down.astype(jnp.float32)

    def one_block(inputs):
        block_rows, block_ids, block_weights = inputs
        slot_ids, source, filled = slot_table(block_ids, expert_count, CAP)
        outgoing = jnp.where(filled[:, None], block_rows[source // top_count], jnp.zeros((), block_rows.dtype))
        outgoing = outgoing.reshape(expert_count, CAP, row_width).astype(jnp.float32)
        gate_part = jnp.einsum('ecd,edf->ecf', outgoing, gate_whole)
        up_part = jnp.einsum('ecd,edf->ecf', outgoing, up_whole)
        copy_hidden = (jax.nn.silu(gate_part) * up_part).astype(jnp.bfloat16)
        results = jnp.einsum('ecf,efd->ecd', copy_hidden.astype(jnp.float32), down_whole)
        picked = results.reshape(expert_count * CAP, row_width)[slot_ids] * block_weights.reshape(-1, 1)
        return lax.optimization_barrier(jnp.sum(picked.reshape(ROWS, top_count, row_width), axis=1))
    routed = lax.map(one_block, (expert_normed.reshape(N_EP, ROWS, row_width), route_ids.reshape(N_EP, ROWS, top_count), route_weights.reshape(N_EP, ROWS, top_count)))
    routed = routed.reshape(expert_rows.shape[0], row_width)
    shared_hidden = (jax.nn.silu(jnp.dot(expert_normed, shared_gate, preferred_element_type=jnp.float32)) * jnp.dot(expert_normed, shared_up, preferred_element_type=jnp.float32)).astype(jnp.bfloat16)
    expert_sum = routed + jnp.dot(shared_hidden, shared_down, preferred_element_type=jnp.float32)
    return rms_scale(expert_sum, expert_scale).astype(jnp.bfloat16)

def reference(mixer_rows, mixer_gain, gate_proj, input_proj, conv_taps, input_gates, decay_gates, decay_offset, out_proj, mixer_scale, expert_rows, expert_gain, route_ids, route_weights, expert_gate, expert_up, expert_down, shared_gate, shared_up, shared_down, expert_scale):
    mixer_out = mixer_half(mixer_rows, mixer_gain, gate_proj, input_proj, conv_taps, input_gates, decay_gates, decay_offset, out_proj, mixer_scale)
    expert_out = expert_half(expert_rows, expert_gain, route_ids, route_weights, expert_gate, expert_up, expert_down, shared_gate, shared_up, shared_down, expert_scale)
    return (mixer_out, expert_out)
```

```python
import functools

import jax
import jax.numpy as jnp
from jax import lax
from jax.experimental import pallas as pl
from jax.experimental.pallas import tpu as pltpu
from jax.sharding import PartitionSpec as P


eps = 1e-06
lru_power = 8.0
bf16 = jnp.bfloat16
f32 = jnp.float32


def vmem():
    return pl.BlockSpec(memory_space=pltpu.VMEM)


def smem():
    return pl.BlockSpec(memory_space=pltpu.SMEM)


def hbm():
    return pl.BlockSpec(memory_space=pltpu.HBM)


def params(mib, micros):
    return dict(
        compiler_params=pltpu.CompilerParams(vmem_limit_bytes=mib * 2**20),
        cost_estimate=pl.CostEstimate(
            flops=int(micros * 1e9), transcendentals=0, bytes_accessed=int(micros * 1e6)
        ),
    )


def normed_block(rows, gain):
    floats = rows.astype(f32)
    return floats * lax.rsqrt(jnp.mean(floats * floats, axis=-1, keepdims=True) + eps) * gain


def norm_part(src, gain, dst, take, put, count, step):
    def one(i, _):
        start = i * step
        dst[pl.ds(pl.multiple_of(put + start, 8), step), :] = normed_block(
            src[pl.ds(pl.multiple_of(take + start, step), step), :], gain
        ).astype(bf16)
        return 0

    lax.fori_loop(0, count // step, one, 0)


def minus_expm1(v):
    series = jnp.ones_like(v)
    for n in (8, 7, 6, 5, 4, 3, 2):
        series = 1.0 + series * v * (1.0 / n)
    return jnp.where(v > -0.35, -v * series, 1.0 - jnp.exp(v))


def mixer_kernel(
    first, rows_hbm, halo, gain, gate_hbm, input_hbm, taps, in_gates, de_gates, offset,
    gate_out, states_out, decay_out, carry_out, rows, normed, weights, sems,
):
    count = rows.shape[0]
    pieces = 4
    part = count // pieces
    loads = [
        pltpu.make_async_copy(
            rows_hbm.at[k * part : (k + 1) * part, :], rows.at[k * part : (k + 1) * part, :], sems.at[k]
        )
        for k in range(pieces)
    ]
    copies = [
        pltpu.make_async_copy(src, weights.at[k], sems.at[pieces + k])
        for k, src in enumerate((input_hbm, gate_hbm))
    ]
    for c in loads + copies:
        c.start()
    pad = halo.shape[0]
    gains = gain[...]
    normed[0:pad, :] = normed_block(halo[...], gains).astype(bf16)
    for k in range(pieces):
        loads[k].wait()
        norm_part(rows, gains, normed, k * part, pad + k * part, part, 16)
    copies[0].wait()
    branch = jnp.dot(normed[...], weights[0], preferred_element_type=f32).astype(bf16).astype(f32)
    tap_count = taps.shape[0]
    conv = None
    for k in range(tap_count):
        back = tap_count - 1 - k
        moved = pltpu.roll(branch, back, 0) if back else branch
        term = taps[k : k + 1, :] * moved
        conv = term if conv is None else conv + term
    conv = conv[pad:, :].astype(bf16)
    width = in_gates.shape[1]
    blocks = in_gates.shape[0]

    def gate(maps):
        return jax.nn.sigmoid(
            jnp.concatenate(
                [
                    jnp.dot(conv[:, b * width : (b + 1) * width], maps[b], preferred_element_type=f32)
                    for b in range(blocks)
                ],
                axis=1,
            )
        )

    input_gate = gate(in_gates)
    decay_gate = gate(de_gates)
    minus_offset = -offset[...]
    softplus = jnp.maximum(minus_offset, 0.0) + jnp.log1p(jnp.exp(-jnp.abs(minus_offset)))
    log_decay = -lru_power * decay_gate * softplus
    row_ids = lax.broadcasted_iota(jnp.int32, log_decay.shape, 0)
    scale = jnp.sqrt(minus_expm1(2.0 * log_decay))
    scale = jnp.where((row_ids == 0) & (first[2] == 0), 1.0, scale)
    state = scale * input_gate * conv.astype(f32)
    decay = jnp.exp(log_decay)
    step = 1
    while step < count:
        keep = row_ids >= step
        before_state = jnp.where(keep, pltpu.roll(state, step, 0), 0.0)
        before_decay = jnp.where(keep, pltpu.roll(decay, step, 0), 1.0)
        state = decay * before_state + state
        decay = decay * before_decay
        step *= 2
    states_out[...] = state
    decay_out[...] = decay
    carry_out[0:1, :] = decay[count - 1 :, :]
    carry_out[1:2, :] = state[count - 1 :, :]
    copies[1].wait()
    gate_out[...] = jax.nn.gelu(
        jnp.dot(normed[pad:, :], weights[1], preferred_element_type=f32)
    )


def mixer_local(first, rows, halo, gain, gate_proj, input_proj, taps, in_gates, de_gates, offset):
    count, width = rows.shape[0], gate_proj.shape[1]
    full = jax.ShapeDtypeStruct((count, width), f32)
    return pl.pallas_call(
        mixer_kernel,
        out_shape=(full, full, full, jax.ShapeDtypeStruct((2, width), f32)),
        in_specs=[smem(), hbm(), vmem(), vmem(), hbm(), hbm(), vmem(), vmem(), vmem(), vmem()],
        out_specs=(vmem(), vmem(), vmem(), vmem()),
        scratch_shapes=[
            pltpu.VMEM(rows.shape, bf16),
            pltpu.VMEM((count + halo.shape[0], rows.shape[1]), bf16),
            pltpu.VMEM((2, *gate_proj.shape), bf16),
            pltpu.SemaphoreType.DMA((6,)),
        ],
        name="mixer_local",
        **params(24, 8),
    )(first, rows, halo, gain, gate_proj, input_proj, taps, in_gates, de_gates, offset)


def front_kernel(
    core, rows_hbm, gain, ids, mixer_hbm, out_hbm, normed_hbm, slots, tail,
    rows, normed, out, sems, *, experts, capacity,
):
    count, _ = rows.shape
    half = out.shape[1]
    pieces = 4
    part = count // pieces
    loads = [
        pltpu.make_async_copy(
            rows_hbm.at[k * part : (k + 1) * part, :], rows.at[k * part : (k + 1) * part, :], sems.at[k]
        )
        for k in range(pieces)
    ]
    last = mixer_hbm.shape[0]
    loads.append(pltpu.make_async_copy(mixer_hbm.at[last - 8 : last, :], tail, sems.at[pieces]))
    for c in loads:
        c.start()
    experts_down = lax.broadcasted_iota(jnp.int32, (experts, count), 0)
    picks = [ids[k : k + 1, :] for k in range(2)]
    hits = [(p == experts_down) for p in picks]
    marks = jnp.where(hits[0] | hits[1], 1.0, 0.0).astype(bf16)
    upper = jnp.where(
        lax.broadcasted_iota(jnp.int32, (count, count), 0)
        < lax.broadcasted_iota(jnp.int32, (count, count), 1),
        1.0,
        0.0,
    ).astype(bf16)
    earlier = jnp.dot(marks, upper, preferred_element_type=f32)
    slots_down = lax.broadcasted_iota(jnp.int32, (experts * capacity, count), 0)
    chosen = None
    for k in range(2):
        place = jnp.sum(jnp.where(hits[k], earlier, 0.0), axis=0, keepdims=True).astype(jnp.int32)
        slot = picks[k] * capacity + place
        slots[k : k + 1, :] = slot
        hit = slot == slots_down
        chosen = hit if chosen is None else chosen | hit
    chosen = jnp.where(chosen, 1.0, 0.0).astype(bf16)
    gains = gain[...]
    saves = []
    for k in range(pieces):
        loads[k].wait()
        norm_part(rows, gains, normed, k * part, k * part, part, 16)
        save = pltpu.make_async_copy(
            normed.at[k * part : (k + 1) * part, :],
            normed_hbm.at[k * part : (k + 1) * part, :],
            sems.at[5 + k],
        )
        save.start()
        saves.append(save)
    mine = normed[:, pl.ds(pl.multiple_of(core[0] * half, half), half)]
    blocks = 3
    size = experts * capacity // blocks
    for k in range(blocks):
        out[k * size : (k + 1) * size, :] = jnp.dot(
            chosen[k * size : (k + 1) * size, :], mine, preferred_element_type=f32
        ).astype(bf16)
        save = pltpu.make_async_copy(
            out.at[k * size : (k + 1) * size, :], out_hbm.at[k * size : (k + 1) * size, :], sems.at[9 + k]
        )
        save.start()
        saves.append(save)
    loads[pieces].wait()
    for c in saves:
        c.wait()


def expert_front(core, rows, gain, ids, mixer_rows, experts, capacity):
    count, width = rows.shape
    return pl.pallas_call(
        functools.partial(front_kernel, experts=experts, capacity=capacity),
        out_shape=(
            jax.ShapeDtypeStruct((experts * capacity, width // 2), bf16),
            jax.ShapeDtypeStruct((count, width), bf16),
            jax.ShapeDtypeStruct((2, count), jnp.int32),
            jax.ShapeDtypeStruct((8, width), bf16),
        ),
        in_specs=[smem(), hbm(), vmem(), vmem(), hbm()],
        out_specs=(hbm(), hbm(), vmem(), vmem()),
        scratch_shapes=[
            pltpu.VMEM((count, width), bf16),
            pltpu.VMEM((count, width), bf16),
            pltpu.VMEM((experts * capacity, width // 2), bf16),
            pltpu.SemaphoreType.DMA((12,)),
        ],
        name="expert_front",
        **params(20, 5),
    )(core, rows, gain, ids, mixer_rows)


def parts_kernel(core, received_hbm, gate, up, out, received, weights, sems, *, whole):
    half, width = weights.shape[0], gate.shape[1]
    start = pl.multiple_of(core[0] * half, half) if whole else 0
    copies = [
        pltpu.make_async_copy(
            src.at[pl.ds(start, half), :], weights.at[:, k * width : (k + 1) * width], sems.at[k]
        )
        for k, src in enumerate((gate, up))
    ]
    pieces = 3
    part = received.shape[0] // pieces
    loads = [
        pltpu.make_async_copy(
            received_hbm.at[k * part : (k + 1) * part, :],
            received.at[k * part : (k + 1) * part, :],
            sems.at[2 + k],
        )
        for k in range(pieces)
    ]
    for c in copies + loads:
        c.start()
    for c in copies:
        c.wait()
    for k in range(pieces):
        loads[k].wait()
        out[k * part : (k + 1) * part, :] = jnp.dot(
            received[k * part : (k + 1) * part, :], weights[...], preferred_element_type=f32
        )


def expert_parts(core, received, gate, up, whole):
    rows, half = received.shape
    width = gate.shape[1]
    return pl.pallas_call(
        functools.partial(parts_kernel, whole=whole),
        out_shape=jax.ShapeDtypeStruct((rows, 2 * width), f32),
        in_specs=[smem(), hbm(), hbm(), hbm()],
        out_specs=vmem(),
        scratch_shapes=[
            pltpu.VMEM(received.shape, bf16),
            pltpu.VMEM((half, 2 * width), bf16),
            pltpu.SemaphoreType.DMA((5,)),
        ],
        name="expert_parts",
        **params(8, 3),
    )(core, received, gate, up)


def prep_kernel(where, gate, up, down, shared, gate_out, up_out, *refs):
    outs, sems = refs[:4], refs[4]
    half, quarter = gate_out.shape[0], outs[0].shape[1]
    size = down.shape[0]
    start = pl.multiple_of((1 - where[0]) * half, half)
    copies = [
        pltpu.make_async_copy(src.at[pl.ds(start, half), :], dst, sems.at[k])
        for k, (src, dst) in enumerate(((gate, gate_out), (up, up_out)))
    ]
    for s in range(4):
        cols = pl.ds(pl.multiple_of(((where[1] + s) % 4) * quarter, quarter), quarter)
        for k, src in enumerate((down, shared)):
            copies.append(
                pltpu.make_async_copy(
                    src.at[:, cols], outs[s].at[k * size : (k + 1) * size, :], sems.at[2 + 2 * s + k]
                )
            )
    for c in copies:
        c.start()
    for c in copies:
        c.wait()


def prepared(where, gate, up, down, shared):
    half, width = gate.shape[0] // 2, gate.shape[1]
    tall = jax.ShapeDtypeStruct((half, width), bf16)
    wide = jax.ShapeDtypeStruct((2 * down.shape[0], down.shape[1] // 4), bf16)
    return pl.pallas_call(
        prep_kernel,
        out_shape=(tall, tall, wide, wide, wide, wide),
        in_specs=[smem()] + [hbm()] * 4,
        out_specs=(hbm(),) * 6,
        scratch_shapes=[pltpu.SemaphoreType.DMA((10,))],
        name="prepared",
        **params(2, 3),
    )(where, gate, up, down, shared)


def down_kernel(core, *refs, at):
    hidden, weights, (keep, send, w, sems) = refs[:4], refs[4:8], refs[8:]
    size = hidden[0].shape[1]
    width = keep.shape[1]
    copies = [
        pltpu.make_async_copy(
            p.at[at : at + size, :], w.at[k * size : (k + 1) * size, :], sems.at[k]
        )
        for k, p in enumerate(weights)
    ]
    for c in copies:
        c.start()
    h = jnp.concatenate([p[...] for p in hidden], axis=1)
    for c in copies:
        c.wait()
    for out, which in ((send, 1 - core[0]), (keep, core[0])):
        cols = pl.ds(pl.multiple_of(which * width, width), width)
        out[...] = jnp.dot(h, w[:, cols], preferred_element_type=f32)


def down_parts(core, hidden, weights, at):
    width = weights[0].shape[1] // 2
    shape = jax.ShapeDtypeStruct((hidden[0].shape[0], width), f32)
    return pl.pallas_call(
        functools.partial(down_kernel, at=at),
        out_shape=(shape, shape),
        in_specs=[smem()] + [vmem()] * 4 + [hbm()] * 4,
        out_specs=(vmem(), vmem()),
        scratch_shapes=[
            pltpu.VMEM((4 * hidden[0].shape[1], 2 * width), bf16),
            pltpu.SemaphoreType.DMA((4,)),
        ],
        name="down_parts",
        **params(10, 2.5),
    )(core, *hidden, *weights)


def mixer_out_kernel(where, gate, states, decays, carries, out_hbm, keep, send, gated, weights, sem):
    load = pltpu.make_async_copy(out_hbm, weights, sem)
    load.start()
    carried = jnp.zeros((1, gate.shape[1]), f32)
    for i in range(carries.shape[0] - 1):
        carried = jnp.where(i < where[2], carries[i, 0:1] * carried + carries[i, 1:2], carried)
    gated[...] = (gate[...] * (states[...] + decays[...] * carried)).astype(bf16)
    rows = keep.shape[0] // 4
    load.wait()
    for out, which in ((send, 1 - where[0]), (keep, where[0])):
        picked = jnp.concatenate(
            [
                gated[pl.ds(pl.multiple_of((2 * i + which) * rows, rows), rows), :]
                for i in range(4)
            ],
            axis=0,
        )
        out[...] = jnp.dot(picked, weights[...], preferred_element_type=f32)


def mixer_out_parts(where, gate, states, decays, carries, out_proj):
    rows, width = gate.shape[0], out_proj.shape[1]
    shape = jax.ShapeDtypeStruct((rows // 2, width), f32)
    return pl.pallas_call(
        mixer_out_kernel,
        out_shape=(shape, shape),
        in_specs=[smem()] + [vmem()] * 4 + [hbm()],
        out_specs=(vmem(), vmem()),
        scratch_shapes=[
            pltpu.VMEM(gate.shape, bf16),
            pltpu.VMEM(out_proj.shape, bf16),
            pltpu.SemaphoreType.DMA,
        ],
        name="mixer_out",
        **params(16, 3),
    )(where, gate, states, decays, carries, out_proj)


def combine_kernel(back, slots, weights, own, other, out):
    down = lax.broadcasted_iota(jnp.int32, (back.shape[0], slots.shape[1]), 0)
    mix = jnp.where(slots[0:1, :] == down, weights[0:1, :], 0.0) + jnp.where(
        slots[1:2, :] == down, weights[1:2, :], 0.0
    )
    out[...] = own[...] + other[...] + lax.dot_general(
        mix, back[...], (((0,), (0,)), ((), ())), preferred_element_type=f32,
        precision=lax.Precision.HIGHEST,
    )


def combined(back, slots, weights, own, other):
    return pl.pallas_call(
        combine_kernel,
        out_shape=jax.ShapeDtypeStruct(own.shape, f32),
        in_specs=[vmem()] * 5,
        out_specs=vmem(),
        name="combine",
        **params(12, 3),
    )(back, slots, weights, own, other)


def rms_scale(values, scale):
    return values * lax.rsqrt(jnp.mean(values * values, axis=-1, keepdims=True) + eps) * scale


def swapped(block):
    return lax.ppermute(block, "tp", [(i, i ^ 1) for i in range(8)])


def turned(block, by):
    return lax.ppermute(block, "tp", [(i, (i + 2 * by) % 8) for i in range(8)])


def after(value, *others):
    return lax.optimization_barrier((value, *others))[0]


def gathered(block):
    return [block] + [turned(block, s) for s in (1, 3, 2)]


def whole_body(
    mixer_rows, mixer_gain, gate_proj, input_proj, conv_taps, input_gates, decay_gates,
    decay_offset, out_proj, mixer_scale, expert_rows, expert_gain, route_ids, route_weights,
    expert_gate, expert_up, expert_down, shared_gate, shared_up, shared_down, expert_scale,
):
    ep_index, tp_index = lax.axis_index("ep"), lax.axis_index("tp")
    core, chip = tp_index % 2, tp_index // 2
    where = jnp.stack([core, chip, ep_index])
    rows, width = mixer_rows.shape
    experts = lax.axis_size("ep")
    capacity = rows * 2 * 3 // (2 * experts)
    half = width // 2
    order = (1, 3, 2)

    outgoing, expert_normed, slots, tail = expert_front(
        where, expert_rows, expert_gain.reshape(1, -1), route_ids.T, mixer_rows, experts, capacity
    )
    halo = lax.ppermute(tail, "ep", [(i, i + 1) for i in range(15)])
    received = lax.all_to_all(
        outgoing.reshape(experts, capacity, half), "ep", 0, 0, tiled=True
    ).reshape(experts * capacity, half)

    send_gate, send_up, *downs = prepared(
        after(where, slots), expert_gate[0], expert_up[0], expert_down[0], shared_down
    )
    shared_hidden = (
        jax.nn.silu(jnp.dot(expert_normed, shared_gate, preferred_element_type=f32))
        * jnp.dot(expert_normed, shared_up, preferred_element_type=f32)
    ).astype(bf16)
    shared_all = gathered(shared_hidden)
    other_gate, other_up = (swapped(w) for w in (send_gate, send_up))
    downs = [downs[0]] + [turned(downs[s], s) for s in order]

    gate_branch, local_states, decay_product, carry = mixer_local(
        after(where, shared_hidden, send_gate), mixer_rows, halo, mixer_gain.reshape(1, -1), gate_proj, input_proj,
        conv_taps, input_gates, decay_gates, decay_offset.reshape(1, -1),
    )
    hidden_width = expert_gate.shape[2]
    shared_keep, shared_send = down_parts(after(where, carry), shared_all, downs, hidden_width)
    shared_other = swapped(shared_send)

    received = after(received, carry, shared_keep, other_gate, other_up)
    other_part = expert_parts(where, received, other_gate, other_up, False)
    own_part = expert_parts(where, received, expert_gate[0], expert_up[0], True)
    parts = own_part + swapped(other_part)
    copy_hidden = (jax.nn.silu(parts[:, :hidden_width]) * parts[:, hidden_width:]).astype(bf16)
    hidden_all = gathered(copy_hidden)
    carry = after(carry, copy_hidden)
    carries = lax.all_to_all(jnp.broadcast_to(carry[None], (experts, *carry.shape)), "ep", 0, 0, tiled=True)
    keep_result, send_result = down_parts(where, hidden_all, downs, 0)
    results = keep_result + swapped(send_result)
    back = lax.all_to_all(
        results.reshape(experts, capacity, -1), "ep", 0, 0, tiled=True
    ).reshape(experts * capacity, -1)

    carries = after(carries, keep_result)
    keep_term, send_term = mixer_out_parts(where, gate_branch, local_states, decay_product, carries, out_proj)
    pair_term = (keep_term + swapped(send_term)).reshape(4, rows // 8, width)
    mixer_sum = lax.dynamic_index_in_dim(pair_term, chip, 0, keepdims=False)
    for s in order:
        mixer_sum = mixer_sum + turned(
            lax.dynamic_index_in_dim(pair_term, (chip + s) % 4, 0, keepdims=False).astype(bf16), s
        ).astype(f32)
    mixer_out = rms_scale(mixer_sum, mixer_scale).astype(bf16)

    expert_sum = combined(back, slots, route_weights.T, shared_keep, shared_other)
    expert_whole = lax.all_to_all(expert_sum, "tp", split_axis=0, concat_axis=1, tiled=True)
    expert_out = rms_scale(expert_whole, expert_scale).astype(bf16)
    return (mixer_out, expert_out)


def solution(mesh):
    placed = (
        P("ep", None), P(), P(None, "tp"), P(None, "tp"), P(None, "tp"), P("tp", None, None),
        P("tp", None, None), P("tp"), P("tp", None), P(), P("ep", None), P(), P("ep", None),
        P("ep", None), P("ep", None, "tp"), P("ep", None, "tp"), P("ep", "tp", None),
        P(None, "tp"), P(None, "tp"), P("tp", None), P(),
    )
    return jax.shard_map(
        whole_body,
        mesh=mesh,
        in_specs=placed,
        out_specs=(P(("ep", "tp"), None), P(("ep", "tp"), None)),
        check_vma=False,
    )
```

```python
import functools

import jax
import jax.numpy as jnp
from jax import lax
from jax.experimental import pallas as pl
from jax.experimental.pallas import tpu as pltpu
from jax.sharding import PartitionSpec as P


eps = 1e-06
lru_power = 8.0
bf16 = jnp.bfloat16
f32 = jnp.float32


def vmem():
    return pl.BlockSpec(memory_space=pltpu.VMEM)


def seat():
    tp = lax.axis_index("tp")
    return tp % 2, tp // 2, lax.axis_index("ep")


def hbm():
    return pl.BlockSpec(memory_space=pl.ANY)


def params(mib, micros):
    return dict(
        compiler_params=pltpu.CompilerParams(vmem_limit_bytes=mib * 2**20),
        cost_estimate=pl.CostEstimate(
            flops=int(micros * 1e9), transcendentals=0, bytes_accessed=int(micros * 1e6)
        ),
    )


def normed_block(rows, gain):
    floats = rows.astype(f32)
    return floats * lax.rsqrt(jnp.mean(floats * floats, axis=-1, keepdims=True) + eps) * gain


def norm_part(src, gain, dst, take, put, count, step):
    def one(i, _):
        start = i * step
        dst[pl.ds(pl.multiple_of(put + start, 8), step), :] = normed_block(
            src[pl.ds(pl.multiple_of(take + start, step), step), :], gain
        ).astype(bf16)
        return 0

    lax.fori_loop(0, count // step, one, 0)


def minus_expm1(v):
    series = jnp.ones_like(v)
    for n in (8, 7, 6, 5, 4, 3, 2):
        series = 1.0 + series * v * (1.0 / n)
    return jnp.where(v > -0.35, -v * series, 1.0 - jnp.exp(v))


def mixer_kernel(
    rows_hbm, halo, gain, gate_hbm, input_hbm, taps, in_gates, de_gates, offset,
    gate_out, states_out, decay_out, carry_out, rows, normed, weights, sems,
):
    count = rows.shape[0]
    pieces = 4
    part = count // pieces
    loads = [
        pltpu.make_async_copy(
            rows_hbm.at[k * part : (k + 1) * part, :], rows.at[k * part : (k + 1) * part, :], sems.at[k]
        )
        for k in range(pieces)
    ]
    copies = [
        pltpu.make_async_copy(src, weights.at[k], sems.at[pieces + k])
        for k, src in enumerate((input_hbm, gate_hbm))
    ]
    for c in loads + copies:
        c.start()
    pad = halo.shape[0]
    gains = gain[...]
    normed[0:pad, :] = normed_block(halo[...], gains).astype(bf16)
    for k in range(pieces):
        loads[k].wait()
        norm_part(rows, gains, normed, k * part, pad + k * part, part, 16)
    copies[0].wait()
    branch = jnp.dot(normed[...], weights[0], preferred_element_type=f32).astype(bf16).astype(f32)
    tap_count = taps.shape[0]
    conv = None
    for k in range(tap_count):
        back = tap_count - 1 - k
        moved = pltpu.roll(branch, back, 0) if back else branch
        term = taps[k : k + 1, :] * moved
        conv = term if conv is None else conv + term
    conv = conv[pad:, :].astype(bf16)
    width = in_gates.shape[1]
    blocks = in_gates.shape[0]

    def gate(maps):
        return jax.nn.sigmoid(
            jnp.concatenate(
                [
                    jnp.dot(conv[:, b * width : (b + 1) * width], maps[b], preferred_element_type=f32)
                    for b in range(blocks)
                ],
                axis=1,
            )
        )

    input_gate = gate(in_gates)
    decay_gate = gate(de_gates)
    minus_offset = -offset[...]
    softplus = jnp.maximum(minus_offset, 0.0) + jnp.log1p(jnp.exp(-jnp.abs(minus_offset)))
    log_decay = -lru_power * decay_gate * softplus
    row_ids = lax.broadcasted_iota(jnp.int32, log_decay.shape, 0)
    scale = jnp.sqrt(minus_expm1(2.0 * log_decay))
    scale = jnp.where((row_ids == 0) & (seat()[2] == 0), 1.0, scale)
    state = scale * input_gate * conv.astype(f32)
    decay = jnp.exp(log_decay)
    step = 1
    while step < count:
        keep = row_ids >= step
        before_state = jnp.where(keep, pltpu.roll(state, step, 0), 0.0)
        before_decay = jnp.where(keep, pltpu.roll(decay, step, 0), 1.0)
        state = decay * before_state + state
        decay = decay * before_decay
        step *= 2
    states_out[...] = state
    decay_out[...] = decay
    carry_out[0:1, :] = decay[count - 1 :, :]
    carry_out[1:2, :] = state[count - 1 :, :]
    copies[1].wait()
    gate_out[...] = jax.nn.gelu(
        jnp.dot(normed[pad:, :], weights[1], preferred_element_type=f32)
    )


def mixer_local(rows, halo, gain, gate_proj, input_proj, taps, in_gates, de_gates, offset):
    count, width = rows.shape[0], gate_proj.shape[1]
    full = jax.ShapeDtypeStruct((count, width), f32)
    return pl.pallas_call(
        mixer_kernel,
        out_shape=(full, full, full, jax.ShapeDtypeStruct((2, width), f32)),
        in_specs=[hbm(), vmem(), vmem(), hbm(), hbm(), vmem(), vmem(), vmem(), vmem()],
        out_specs=(vmem(), vmem(), vmem(), vmem()),
        scratch_shapes=[
            pltpu.VMEM(rows.shape, bf16),
            pltpu.VMEM((count + halo.shape[0], rows.shape[1]), bf16),
            pltpu.VMEM((2, *gate_proj.shape), bf16),
            pltpu.SemaphoreType.DMA((6,)),
        ],
        name="mixer_local",
        **params(58, 8),
    )(rows, halo, gain, gate_proj, input_proj, taps, in_gates, de_gates, offset)


def front_kernel(
    rows_hbm, gain, ids, mixer_hbm, out_hbm, normed_hbm, slots, tail,
    rows, normed, out, sems, *, experts, capacity,
):
    count, _ = rows.shape
    half = out.shape[1]
    pieces = 4
    part = count // pieces
    loads = [
        pltpu.make_async_copy(
            rows_hbm.at[k * part : (k + 1) * part, :], rows.at[k * part : (k + 1) * part, :], sems.at[k]
        )
        for k in range(pieces)
    ]
    last = mixer_hbm.shape[0]
    loads.append(pltpu.make_async_copy(mixer_hbm.at[last - 8 : last, :], tail, sems.at[pieces]))
    for c in loads:
        c.start()
    experts_down = lax.broadcasted_iota(jnp.int32, (experts, count), 0)
    picks = [ids[k : k + 1, :] for k in range(2)]
    hits = [(p == experts_down) for p in picks]
    marks = jnp.where(hits[0] | hits[1], 1.0, 0.0).astype(bf16)
    upper = jnp.where(
        lax.broadcasted_iota(jnp.int32, (count, count), 0)
        < lax.broadcasted_iota(jnp.int32, (count, count), 1),
        1.0,
        0.0,
    ).astype(bf16)
    earlier = jnp.dot(marks, upper, preferred_element_type=f32)
    slots_down = lax.broadcasted_iota(jnp.int32, (experts * capacity, count), 0)
    chosen = None
    for k in range(2):
        place = jnp.sum(jnp.where(hits[k], earlier, 0.0), axis=0, keepdims=True).astype(jnp.int32)
        slot = picks[k] * capacity + place
        slots[k : k + 1, :] = slot
        hit = slot == slots_down
        chosen = hit if chosen is None else chosen | hit
    chosen = jnp.where(chosen, 1.0, 0.0).astype(bf16)
    gains = gain[...]
    saves = []
    for k in range(pieces):
        loads[k].wait()
        norm_part(rows, gains, normed, k * part, k * part, part, 16)
        save = pltpu.make_async_copy(
            normed.at[k * part : (k + 1) * part, :],
            normed_hbm.at[k * part : (k + 1) * part, :],
            sems.at[5 + k],
        )
        save.start()
        saves.append(save)
    mine = normed[:, pl.ds(pl.multiple_of(seat()[0] * half, half), half)]
    blocks = 3
    size = experts * capacity // blocks
    for k in range(blocks):
        out[k * size : (k + 1) * size, :] = jnp.dot(
            chosen[k * size : (k + 1) * size, :], mine, preferred_element_type=f32
        ).astype(bf16)
        save = pltpu.make_async_copy(
            out.at[k * size : (k + 1) * size, :], out_hbm.at[k * size : (k + 1) * size, :], sems.at[9 + k]
        )
        save.start()
        saves.append(save)
    loads[pieces].wait()
    for c in saves:
        c.wait()


def expert_front(rows, gain, ids, mixer_rows, experts, capacity):
    count, width = rows.shape
    return pl.pallas_call(
        functools.partial(front_kernel, experts=experts, capacity=capacity),
        out_shape=(
            jax.ShapeDtypeStruct((experts * capacity, width // 2), bf16),
            jax.ShapeDtypeStruct((count, width), bf16),
            jax.ShapeDtypeStruct((2, count), jnp.int32),
            jax.ShapeDtypeStruct((8, width), bf16),
        ),
        in_specs=[hbm(), vmem(), vmem(), hbm()],
        out_specs=(hbm(), hbm(), vmem(), vmem()),
        scratch_shapes=[
            pltpu.VMEM((count, width), bf16),
            pltpu.VMEM((count, width), bf16),
            pltpu.VMEM((experts * capacity, width // 2), bf16),
            pltpu.SemaphoreType.DMA((12,)),
        ],
        name="expert_front",
        **params(58, 5),
    )(rows, gain, ids, mixer_rows)


def parts_kernel(received_hbm, *refs):
    sources, (keep, send, received, weights, sems) = refs[:4], refs[4:]
    half, width = weights.shape[0], sources[0].shape[1]
    start = pl.multiple_of(seat()[0] * half, half)
    copies = []
    for k, src in enumerate(sources):
        rows = pl.ds(start, half) if src.shape[0] > half else pl.ds(0, half)
        copies.append(
            pltpu.make_async_copy(
                src.at[rows, :], weights.at[:, k * width : (k + 1) * width], sems.at[k]
            )
        )
    pieces = 4
    part = received.shape[0] // pieces
    loads = [
        pltpu.make_async_copy(
            received_hbm.at[k * part : (k + 1) * part, :],
            received.at[k * part : (k + 1) * part, :],
            sems.at[4 + k],
        )
        for k in range(pieces)
    ]
    for c in copies + loads:
        c.start()
    for c in copies:
        c.wait()
    for k in range(pieces):
        loads[k].wait()
        both = jnp.dot(
            received[k * part : (k + 1) * part, :], weights[...], preferred_element_type=f32
        )
        keep[k * part : (k + 1) * part, :] = both[:, : 2 * width]
        send[k * part : (k + 1) * part, :] = both[:, 2 * width :]


def expert_parts(received, *weights):
    rows, half = received.shape
    width = weights[0].shape[1]
    shape = jax.ShapeDtypeStruct((rows, 2 * width), f32)
    return pl.pallas_call(
        parts_kernel,
        out_shape=(shape, shape),
        in_specs=[hbm()] * 5,
        out_specs=(vmem(), vmem()),
        scratch_shapes=[
            pltpu.VMEM(received.shape, bf16),
            pltpu.VMEM((half, 4 * width), bf16),
            pltpu.SemaphoreType.DMA((8,)),
        ],
        name="expert_parts",
        **params(12, 5),
    )(received, *weights)


def prep_kernel(gate, up, down, shared, gate_out, up_out, *refs):
    outs, (tall, wide, sems) = refs[:4], refs[4:]
    half, quarter = gate_out.shape[0], outs[0].shape[1]
    size = down.shape[0]
    core, chip, _ = seat()
    start = pl.multiple_of((1 - core) * half, half)
    moves = [
        ((src.at[pl.ds(start, half), :], tall.at[k]),) for k, src in enumerate((gate, up))
    ]
    targets = [(tall.at[0], gate_out), (tall.at[1], up_out)]
    for s in range(4):
        cols = pl.ds(pl.multiple_of(((chip + s) % 4) * quarter, quarter), quarter)
        moves.append(
            tuple(
                (src.at[:, cols], wide.at[s, k * size : (k + 1) * size, :])
                for k, src in enumerate((down, shared))
            )
        )
        targets.append((wide.at[s], outs[s]))
    loads, n = [], 0
    for group in moves:
        made = []
        for src, dst in group:
            made.append(pltpu.make_async_copy(src, dst, sems.at[n]))
            made[-1].start()
            n += 1
        loads.append(made)
    saves = []
    for made, (src, dst) in zip(loads, targets):
        for c in made:
            c.wait()
        saves.append(pltpu.make_async_copy(src, dst, sems.at[n]))
        saves[-1].start()
        n += 1
    for c in saves:
        c.wait()


def prepared(gate, up, down, shared):
    half, width = gate.shape[0] // 2, gate.shape[1]
    tall = jax.ShapeDtypeStruct((half, width), bf16)
    wide = jax.ShapeDtypeStruct((2 * down.shape[0], down.shape[1] // 4), bf16)
    return pl.pallas_call(
        prep_kernel,
        out_shape=(tall, tall, wide, wide, wide, wide),
        in_specs=[hbm()] * 4,
        out_specs=(hbm(),) * 6,
        scratch_shapes=[
            pltpu.VMEM((2, *tall.shape), bf16),
            pltpu.VMEM((4, *wide.shape), bf16),
            pltpu.SemaphoreType.DMA((16,)),
        ],
        name="prepared",
        **params(58, 3),
    )(gate, up, down, shared)


def down_kernel(*refs, at):
    hidden, weights, (keep, send, w, sems) = refs[:4], refs[4:8], refs[8:]
    size = hidden[0].shape[1]
    width = keep.shape[1]
    copies = [
        pltpu.make_async_copy(
            p.at[at : at + size, :], w.at[k * size : (k + 1) * size, :], sems.at[k]
        )
        for k, p in enumerate(weights)
    ]
    for c in copies:
        c.start()
    h = jnp.concatenate([p[...] for p in hidden], axis=1)
    for c in copies:
        c.wait()
    for out, which in ((send, 1 - seat()[0]), (keep, seat()[0])):
        cols = pl.ds(pl.multiple_of(which * width, width), width)
        out[...] = jnp.dot(h, w[:, cols], preferred_element_type=f32)


def down_parts(hidden, weights, at):
    width = weights[0].shape[1] // 2
    shape = jax.ShapeDtypeStruct((hidden[0].shape[0], width), f32)
    return pl.pallas_call(
        functools.partial(down_kernel, at=at),
        out_shape=(shape, shape),
        in_specs=[vmem()] * 4 + [hbm()] * 4,
        out_specs=(vmem(), vmem()),
        scratch_shapes=[
            pltpu.VMEM((4 * hidden[0].shape[1], 2 * width), bf16),
            pltpu.SemaphoreType.DMA((4,)),
        ],
        name="down_parts",
        **params(10, 2.5),
    )(*hidden, *weights)


def mixer_out_kernel(
    gate_hbm, states_hbm, decays_hbm, carries, out_hbm, keep_hbm, send_hbm,
    gate, states, decays, weights, gated, keep, send, sems,
):
    core, _, ep = seat()
    loads = [
        pltpu.make_async_copy(src, dst, sems.at[k])
        for k, (src, dst) in enumerate(((gate_hbm, gate), (states_hbm, states), (decays_hbm, decays)))
    ]
    pieces = 4
    part = keep.shape[1] // pieces
    spans = [slice(k * part, (k + 1) * part) for k in range(pieces)]
    for k, span in enumerate(spans):
        loads.append(pltpu.make_async_copy(out_hbm.at[:, span], weights.at[:, span], sems.at[3 + k]))
    for c in loads:
        c.start()
    carried = jnp.zeros((1, gate.shape[1]), f32)
    for i in range(carries.shape[0] - 1):
        carried = jnp.where(i < ep, carries[i, 0:1] * carried + carries[i, 1:2], carried)
    for c in loads[:3]:
        c.wait()
    values = (gate[...] * (states[...] + decays[...] * carried)).astype(bf16)
    rows = keep.shape[0] // 4
    for i in range(8):
        target = pl.multiple_of(jnp.where(core == i % 2, 4 + i // 2, i // 2) * rows, rows)
        gated[pl.ds(target, rows), :] = values[i * rows : (i + 1) * rows, :]
    saves = []
    for k, span in enumerate(spans):
        loads[3 + k].wait()
        both = jnp.dot(gated[...], weights[:, span], preferred_element_type=f32)
        send[:, span] = both[: 4 * rows]
        keep[:, span] = both[4 * rows :]
        for j, (src, dst) in enumerate(((send, send_hbm), (keep, keep_hbm))):
            saves.append(
                pltpu.make_async_copy(src.at[:, span], dst.at[:, span], sems.at[7 + 2 * k + j])
            )
            saves[-1].start()
    for c in saves:
        c.wait()


def mixer_out_parts(gate, states, decays, carries, out_proj):
    rows, width = gate.shape[0], out_proj.shape[1]
    shape = jax.ShapeDtypeStruct((rows // 2, width), f32)
    return pl.pallas_call(
        mixer_out_kernel,
        out_shape=(shape, shape),
        in_specs=[hbm(), hbm(), hbm(), vmem(), hbm()],
        out_specs=(hbm(), hbm()),
        scratch_shapes=[pltpu.VMEM(gate.shape, f32)] * 3
        + [
            pltpu.VMEM(out_proj.shape, bf16),
            pltpu.VMEM(gate.shape, bf16),
            pltpu.VMEM(shape.shape, f32),
            pltpu.VMEM(shape.shape, f32),
            pltpu.SemaphoreType.DMA((15,)),
        ],
        name="mixer_out",
        **params(58, 3),
    )(gate, states, decays, carries, out_proj)


def combine_kernel(back, slots, weights, own, other, out):
    count = slots.shape[1]
    down = lax.broadcasted_iota(jnp.int32, (back.shape[0], count), 0)
    same = lax.broadcasted_iota(jnp.int32, (count, count), 0) == lax.broadcasted_iota(
        jnp.int32, (count, count), 1
    )
    total = own[...] + other[...]
    for k in range(2):
        hit = jnp.where(slots[k : k + 1, :] == down, 1.0, 0.0).astype(bf16)
        picked = lax.dot_general(
            hit, back[...], (((0,), (0,)), ((), ())), preferred_element_type=f32
        )
        weight = jnp.sum(jnp.where(same, weights[k : k + 1, :], 0.0), axis=1, keepdims=True)
        total = total + weight * picked
    out[...] = total


def combined(back, slots, weights, own, other):
    return pl.pallas_call(
        combine_kernel,
        out_shape=jax.ShapeDtypeStruct(own.shape, f32),
        in_specs=[vmem()] * 5,
        out_specs=vmem(),
        name="combine",
        **params(12, 3),
    )(back, slots, weights, own, other)


def rms_scale(values, scale):
    return values * lax.rsqrt(jnp.mean(values * values, axis=-1, keepdims=True) + eps) * scale


def swapped(block):
    return lax.ppermute(block, "tp", [(i, i ^ 1) for i in range(8)])


def turned(block, by):
    return lax.ppermute(block, "tp", [(i, (i + 2 * by) % 8) for i in range(8)])


def after(value, *others):
    return lax.optimization_barrier((value, *others))[0]


def gathered(block):
    return [block] + [turned(block, s) for s in (1, 3, 2)]


def whole_body(
    mixer_rows, mixer_gain, gate_proj, input_proj, conv_taps, input_gates, decay_gates,
    decay_offset, out_proj, mixer_scale, expert_rows, expert_gain, route_ids, route_weights,
    expert_gate, expert_up, expert_down, shared_gate, shared_up, shared_down, expert_scale,
):
    tp_index = lax.axis_index("tp")
    chip = tp_index // 2
    rows, width = mixer_rows.shape
    experts = lax.axis_size("ep")
    capacity = rows * 2 * 3 // (2 * experts)
    half = width // 2
    order = (1, 3, 2)

    outgoing, expert_normed, slots, tail = expert_front(
        expert_rows, expert_gain.reshape(1, -1), route_ids.T, mixer_rows, experts, capacity
    )
    halo = lax.ppermute(tail, "ep", [(i, i + 1) for i in range(15)])
    received = lax.all_to_all(
        outgoing.reshape(experts, capacity, half), "ep", 0, 0, tiled=True
    ).reshape(experts * capacity, half)

    send_gate, send_up, *downs = prepared(
        expert_gate[0], expert_up[0], after(expert_down[0], slots), shared_down
    )
    shared_hidden = (
        jax.nn.silu(jnp.dot(expert_normed, shared_gate, preferred_element_type=f32))
        * jnp.dot(expert_normed, shared_up, preferred_element_type=f32)
    ).astype(bf16)
    shared_all = gathered(shared_hidden)
    other_gate, other_up = (swapped(w) for w in (send_gate, send_up))
    downs = [downs[0]] + [turned(downs[s], s) for s in order]

    gate_branch, local_states, decay_product, carry = mixer_local(
        after(mixer_rows, shared_hidden, send_gate), halo, mixer_gain.reshape(1, -1), gate_proj, input_proj,
        conv_taps, input_gates, decay_gates, decay_offset.reshape(1, -1),
    )
    hidden_width = expert_gate.shape[2]
    received = after(received, carry)
    own_part, other_part = expert_parts(
        received, expert_gate[0], expert_up[0], other_gate, other_up
    )
    parts = own_part + swapped(other_part)
    copy_hidden = (jax.nn.silu(parts[:, :hidden_width]) * parts[:, hidden_width:]).astype(bf16)
    hidden_all = gathered(copy_hidden)
    carry = after(carry, copy_hidden)
    carries = lax.all_to_all(
        jnp.broadcast_to(carry[None], (experts, *carry.shape)), "ep", 0, 0, tiled=True
    )
    keep_result, send_result = down_parts(hidden_all, downs, 0)
    results = (keep_result + swapped(send_result)).astype(bf16)
    shared_keep, shared_send = down_parts(
        [after(shared_all[0], results), *shared_all[1:]], downs, hidden_width
    )
    shared_other = swapped(shared_send)
    back = lax.all_to_all(
        results.reshape(experts, capacity, -1), "ep", 0, 0, tiled=True
    ).reshape(experts * capacity, -1)

    carries = after(carries, keep_result)
    keep_term, send_term = mixer_out_parts(
        gate_branch, local_states, decay_product, carries, out_proj
    )
    pair_term = (keep_term + swapped(send_term)).reshape(4, rows // 8, width)
    mixer_sum = lax.dynamic_index_in_dim(pair_term, chip, 0, keepdims=False)
    for s in order:
        mixer_sum = mixer_sum + turned(
            lax.dynamic_index_in_dim(pair_term, (chip + s) % 4, 0, keepdims=False).astype(bf16), s
        ).astype(f32)
    mixer_out = rms_scale(mixer_sum, mixer_scale).astype(bf16)

    expert_sum = combined(back, slots, route_weights.T, shared_keep, shared_other)
    expert_whole = lax.all_to_all(expert_sum, "tp", split_axis=0, concat_axis=1, tiled=True)
    expert_out = rms_scale(expert_whole, expert_scale).astype(bf16)
    return (mixer_out, expert_out)


def solution(mesh):
    placed = (
        P("ep", None), P(), P(None, "tp"), P(None, "tp"), P(None, "tp"), P("tp", None, None),
        P("tp", None, None), P("tp"), P("tp", None), P(), P("ep", None), P(), P("ep", None),
        P("ep", None), P("ep", None, "tp"), P("ep", None, "tp"), P("ep", "tp", None),
        P(None, "tp"), P(None, "tp"), P("tp", None), P(),
    )
    return jax.shard_map(
        whole_body,
        mesh=mesh,
        in_specs=placed,
        out_specs=(P(("ep", "tp"), None), P(("ep", "tp"), None)),
        check_vma=False,
    )
```

```python
import functools

import jax
import jax.numpy as jnp
from jax import lax
from jax.experimental import pallas as pl
from jax.experimental.pallas import tpu as pltpu
from jax.sharding import PartitionSpec as P


eps = 1e-06
lru_power = 8.0
bf16 = jnp.bfloat16
f32 = jnp.float32


def vmem():
    return pl.BlockSpec(memory_space=pltpu.VMEM)


def seat():
    tp = lax.axis_index("tp")
    return tp % 2, tp // 2, lax.axis_index("ep")


def hbm():
    return pl.BlockSpec(memory_space=pl.ANY)


def params(mib, micros):
    return dict(
        compiler_params=pltpu.CompilerParams(vmem_limit_bytes=mib * 2**20),
        cost_estimate=pl.CostEstimate(
            flops=int(micros * 1e9), transcendentals=0, bytes_accessed=int(micros * 1e6)
        ),
    )


def normed_block(rows, gain):
    floats = rows.astype(f32)
    return floats * lax.rsqrt(jnp.mean(floats * floats, axis=-1, keepdims=True) + eps) * gain


def norm_part(src, gain, dst, take, put, count, step):
    def one(i, _):
        start = i * step
        dst[pl.ds(pl.multiple_of(put + start, 8), step), :] = normed_block(
            src[pl.ds(pl.multiple_of(take + start, step), step), :], gain
        ).astype(bf16)
        return 0

    lax.fori_loop(0, count // step, one, 0)


def minus_expm1(v):
    series = jnp.ones_like(v)
    for n in (8, 7, 6, 5, 4, 3, 2):
        series = 1.0 + series * v * (1.0 / n)
    return jnp.where(v > -0.35, -v * series, 1.0 - jnp.exp(v))


def mixer_kernel(
    rows_hbm, halo, gain, gate_hbm, input_hbm, taps, in_gates, de_gates, offset,
    gate_out, states_out, decay_out, carry_out, rows, normed, weights, sems,
):
    count = rows.shape[0]
    pieces = 4
    part = count // pieces
    loads = [
        pltpu.make_async_copy(
            rows_hbm.at[k * part : (k + 1) * part, :], rows.at[k * part : (k + 1) * part, :], sems.at[k]
        )
        for k in range(pieces)
    ]
    copies = [
        pltpu.make_async_copy(src, weights.at[k], sems.at[pieces + k])
        for k, src in enumerate((input_hbm, gate_hbm))
    ]
    for c in loads + copies:
        c.start()
    pad = halo.shape[0]
    gains = gain[...]
    normed[0:pad, :] = normed_block(halo[...], gains).astype(bf16)
    for k in range(pieces):
        loads[k].wait()
        norm_part(rows, gains, normed, k * part, pad + k * part, part, 32)
    copies[0].wait()
    branch = jnp.dot(normed[...], weights[0], preferred_element_type=f32).astype(bf16).astype(f32)
    tap_count = taps.shape[0]
    conv = None
    for k in range(tap_count):
        back = tap_count - 1 - k
        moved = pltpu.roll(branch, back, 0) if back else branch
        term = taps[k : k + 1, :] * moved
        conv = term if conv is None else conv + term
    conv = conv[pad:, :].astype(bf16)
    width = in_gates.shape[1]
    blocks = in_gates.shape[0]

    def gate(maps):
        return jax.nn.sigmoid(
            jnp.concatenate(
                [
                    jnp.dot(conv[:, b * width : (b + 1) * width], maps[b], preferred_element_type=f32)
                    for b in range(blocks)
                ],
                axis=1,
            )
        )

    input_gate = gate(in_gates)
    decay_gate = gate(de_gates)
    minus_offset = -offset[...]
    softplus = jnp.maximum(minus_offset, 0.0) + jnp.log1p(jnp.exp(-jnp.abs(minus_offset)))
    log_decay = -lru_power * decay_gate * softplus
    row_ids = lax.broadcasted_iota(jnp.int32, log_decay.shape, 0)
    scale = jnp.sqrt(minus_expm1(2.0 * log_decay))
    scale = jnp.where((row_ids == 0) & (seat()[2] == 0), 1.0, scale)
    state = scale * input_gate * conv.astype(f32)
    decay = jnp.exp(log_decay)
    step = 1
    while step < count:
        keep = row_ids >= step
        before_state = jnp.where(keep, pltpu.roll(state, step, 0), 0.0)
        before_decay = jnp.where(keep, pltpu.roll(decay, step, 0), 1.0)
        state = decay * before_state + state
        decay = decay * before_decay
        step *= 2
    states_out[...] = state
    decay_out[...] = decay
    carry_out[0:1, :] = decay[count - 1 :, :]
    carry_out[1:2, :] = state[count - 1 :, :]
    copies[1].wait()
    gate_out[...] = jax.nn.gelu(
        jnp.dot(normed[pad:, :], weights[1], preferred_element_type=f32)
    )


def mixer_local(rows, halo, gain, gate_proj, input_proj, taps, in_gates, de_gates, offset):
    count, width = rows.shape[0], gate_proj.shape[1]
    full = jax.ShapeDtypeStruct((count, width), f32)
    return pl.pallas_call(
        mixer_kernel,
        out_shape=(full, full, full, jax.ShapeDtypeStruct((2, width), f32)),
        in_specs=[hbm(), vmem(), vmem(), hbm(), hbm(), vmem(), vmem(), vmem(), vmem()],
        out_specs=(vmem(), vmem(), vmem(), vmem()),
        scratch_shapes=[
            pltpu.VMEM(rows.shape, bf16),
            pltpu.VMEM((count + halo.shape[0], rows.shape[1]), bf16),
            pltpu.VMEM((2, *gate_proj.shape), bf16),
            pltpu.SemaphoreType.DMA((6,)),
        ],
        name="mixer_local",
        **params(58, 8),
    )(rows, halo, gain, gate_proj, input_proj, taps, in_gates, de_gates, offset)


def front_kernel(
    rows_hbm, gain, ids, mixer_hbm, out_hbm, normed_hbm, slots, tail,
    rows, normed, out, sems, *, experts, capacity,
):
    count, _ = rows.shape
    half = out.shape[1]
    pieces = 4
    part = count // pieces
    loads = [
        pltpu.make_async_copy(
            rows_hbm.at[k * part : (k + 1) * part, :], rows.at[k * part : (k + 1) * part, :], sems.at[k]
        )
        for k in range(pieces)
    ]
    last = mixer_hbm.shape[0]
    loads.append(pltpu.make_async_copy(mixer_hbm.at[last - 8 : last, :], tail, sems.at[pieces]))
    for c in loads:
        c.start()
    experts_down = lax.broadcasted_iota(jnp.int32, (experts, count), 0)
    picks = [ids[k : k + 1, :] for k in range(2)]
    hits = [(p == experts_down) for p in picks]
    marks = jnp.where(hits[0] | hits[1], 1.0, 0.0).astype(bf16)
    upper = jnp.where(
        lax.broadcasted_iota(jnp.int32, (count, count), 0)
        < lax.broadcasted_iota(jnp.int32, (count, count), 1),
        1.0,
        0.0,
    ).astype(bf16)
    earlier = jnp.dot(marks, upper, preferred_element_type=f32)
    slots_down = lax.broadcasted_iota(jnp.int32, (experts * capacity, count), 0)
    chosen = None
    for k in range(2):
        place = jnp.sum(jnp.where(hits[k], earlier, 0.0), axis=0, keepdims=True).astype(jnp.int32)
        slot = picks[k] * capacity + place
        slots[k : k + 1, :] = slot
        hit = slot == slots_down
        chosen = hit if chosen is None else chosen | hit
    chosen = jnp.where(chosen, 1.0, 0.0).astype(bf16)
    gains = gain[...]
    saves = []
    for k in range(pieces):
        loads[k].wait()
        norm_part(rows, gains, normed, k * part, k * part, part, 64)
        save = pltpu.make_async_copy(
            normed.at[k * part : (k + 1) * part, :],
            normed_hbm.at[k * part : (k + 1) * part, :],
            sems.at[5 + k],
        )
        save.start()
        saves.append(save)
    mine = normed[:, pl.ds(pl.multiple_of(seat()[0] * half, half), half)]
    blocks = 3
    size = experts * capacity // blocks
    for k in range(blocks):
        out[k * size : (k + 1) * size, :] = jnp.dot(
            chosen[k * size : (k + 1) * size, :], mine, preferred_element_type=f32
        ).astype(bf16)
        save = pltpu.make_async_copy(
            out.at[k * size : (k + 1) * size, :], out_hbm.at[k * size : (k + 1) * size, :], sems.at[9 + k]
        )
        save.start()
        saves.append(save)
    loads[pieces].wait()
    for c in saves:
        c.wait()


def expert_front(rows, gain, ids, mixer_rows, experts, capacity):
    count, width = rows.shape
    return pl.pallas_call(
        functools.partial(front_kernel, experts=experts, capacity=capacity),
        out_shape=(
            jax.ShapeDtypeStruct((experts * capacity, width // 2), bf16),
            jax.ShapeDtypeStruct((count, width), bf16),
            jax.ShapeDtypeStruct((2, count), jnp.int32),
            jax.ShapeDtypeStruct((8, width), bf16),
        ),
        in_specs=[hbm(), vmem(), vmem(), hbm()],
        out_specs=(hbm(), hbm(), vmem(), vmem()),
        scratch_shapes=[
            pltpu.VMEM((count, width), bf16),
            pltpu.VMEM((count, width), bf16),
            pltpu.VMEM((experts * capacity, width // 2), bf16),
            pltpu.SemaphoreType.DMA((12,)),
        ],
        name="expert_front",
        **params(58, 5),
    )(rows, gain, ids, mixer_rows)


def parts_kernel(received_hbm, *refs):
    sources, other, (keep, send, received, weights, sems) = refs[:2], refs[2], refs[3:]
    half, width = weights.shape[0], sources[0].shape[1]
    start = pl.multiple_of(seat()[0] * half, half)
    blocks = [src.at[pl.ds(start, half), :] for src in sources] + [other.at[0], other.at[1]]
    copies = [
        pltpu.make_async_copy(src, weights.at[:, k * width : (k + 1) * width], sems.at[k])
        for k, src in enumerate(blocks)
    ]
    pieces = 4
    part = received.shape[0] // pieces
    loads = [
        pltpu.make_async_copy(
            received_hbm.at[k * part : (k + 1) * part, :],
            received.at[k * part : (k + 1) * part, :],
            sems.at[4 + k],
        )
        for k in range(pieces)
    ]
    for c in copies + loads:
        c.start()
    for c in copies:
        c.wait()
    for k in range(pieces):
        loads[k].wait()
        both = jnp.dot(
            received[k * part : (k + 1) * part, :], weights[...], preferred_element_type=f32
        )
        keep[k * part : (k + 1) * part, :] = both[:, : 2 * width]
        send[k * part : (k + 1) * part, :] = both[:, 2 * width :]


def expert_parts(received, *weights):
    rows, half = received.shape
    width = weights[0].shape[1]
    shape = jax.ShapeDtypeStruct((rows, 2 * width), f32)
    return pl.pallas_call(
        parts_kernel,
        out_shape=(shape, shape),
        in_specs=[hbm()] * 4,
        out_specs=(vmem(), vmem()),
        scratch_shapes=[
            pltpu.VMEM(received.shape, bf16),
            pltpu.VMEM((half, 4 * width), bf16),
            pltpu.SemaphoreType.DMA((8,)),
        ],
        name="expert_parts",
        **params(12, 5),
    )(received, *weights)


def prep_kernel(gate, up, down, shared, tall_out, *refs):
    keeps, (send, tall, wide, sems) = refs[:4], refs[4:]
    half, eighth = tall_out.shape[1], send.shape[2]
    size = down.shape[0]
    core, chip, _ = seat()
    start = pl.multiple_of((1 - core) * half, half)
    moves = []
    for c in range(2):
        for s in range(4):
            at = (2 * ((chip + s) % 4) + (1 - core if c == 0 else core)) * eighth
            cols = pl.ds(pl.multiple_of(at, eighth), eighth)
            moves.append(
                tuple(
                    (src.at[:, cols], wide.at[c, s, k * size : (k + 1) * size, :])
                    for k, src in enumerate((down, shared))
                )
            )
    moves = [
        tuple((src.at[pl.ds(start, half), :], tall.at[k]) for k, src in enumerate((gate, up)))
    ] + moves
    targets = [(tall, tall_out)] + [(wide.at[0, s], send.at[s]) for s in range(4)]
    targets += [(wide.at[1, s], keeps[s]) for s in range(4)]
    loads, n = [], 0
    for group in moves:
        made = []
        for src, dst in group:
            made.append(pltpu.make_async_copy(src, dst, sems.at[n]))
            made[-1].start()
            n += 1
        loads.append(made)
    saves = []
    for made, (src, dst) in zip(loads, targets):
        for c in made:
            c.wait()
        saves.append(pltpu.make_async_copy(src, dst, sems.at[n]))
        saves[-1].start()
        n += 1
    for c in saves:
        c.wait()


def prepared(gate, up, down, shared):
    half, width = gate.shape[0] // 2, gate.shape[1]
    tall = jax.ShapeDtypeStruct((2, half, width), bf16)
    wide = jax.ShapeDtypeStruct((2 * down.shape[0], down.shape[1] // 8), bf16)
    send = jax.ShapeDtypeStruct((4, *wide.shape), bf16)
    return pl.pallas_call(
        prep_kernel,
        out_shape=(tall, wide, wide, wide, wide, send),
        in_specs=[hbm()] * 4,
        out_specs=(hbm(),) * 6,
        scratch_shapes=[
            pltpu.VMEM(tall.shape, bf16),
            pltpu.VMEM((2, 4, *wide.shape), bf16),
            pltpu.SemaphoreType.DMA((27,)),
        ],
        name="prepared",
        **params(58, 3),
    )(gate, up, down, shared)


def down_kernel(*refs, at):
    hidden, weights, (out, w, sems) = refs[:8], refs[8:16], refs[16:]
    size = hidden[0].shape[1]
    copies = [
        pltpu.make_async_copy(
            p.at[at : at + size, :], w.at[k * size : (k + 1) * size, :], sems.at[k]
        )
        for k, p in enumerate(weights)
    ]
    for c in copies:
        c.start()
    h = jnp.concatenate([p[...] for p in hidden], axis=1)
    for c in copies:
        c.wait()
    out[...] = jnp.dot(h, w[...], preferred_element_type=f32).astype(out.dtype)


def down_projected(hidden, weights, at, kind):
    width = weights[0].shape[1]
    return pl.pallas_call(
        functools.partial(down_kernel, at=at),
        out_shape=jax.ShapeDtypeStruct((hidden[0].shape[0], width), kind),
        in_specs=[vmem()] * 8 + [hbm()] * 8,
        out_specs=vmem(),
        scratch_shapes=[
            pltpu.VMEM((8 * hidden[0].shape[1], width), bf16),
            pltpu.SemaphoreType.DMA((8,)),
        ],
        name="down_projected",
        **params(10, 2.5),
    )(*hidden, *weights)


def mixer_out_kernel(
    gate_hbm, states_hbm, decays_hbm, carries, out_hbm, keep_hbm, send_hbm,
    gate, states, decays, weights, gated, keep, send, sems,
):
    core, _, ep = seat()
    loads = [
        pltpu.make_async_copy(src, dst, sems.at[k])
        for k, (src, dst) in enumerate(((gate_hbm, gate), (states_hbm, states), (decays_hbm, decays)))
    ]
    pieces = 4
    part = keep.shape[1] // pieces
    spans = [slice(k * part, (k + 1) * part) for k in range(pieces)]
    for k, span in enumerate(spans):
        loads.append(pltpu.make_async_copy(out_hbm.at[:, span], weights.at[:, span], sems.at[3 + k]))
    for c in loads:
        c.start()
    carried = jnp.zeros((1, gate.shape[1]), f32)
    for i in range(carries.shape[0] - 1):
        carried = jnp.where(i < ep, carries[i, 0:1] * carried + carries[i, 1:2], carried)
    for c in loads[:3]:
        c.wait()
    values = (gate[...] * (states[...] + decays[...] * carried)).astype(bf16)
    rows = keep.shape[0] // 4
    for i in range(8):
        target = pl.multiple_of(jnp.where(core == i % 2, 4 + i // 2, i // 2) * rows, rows)
        gated[pl.ds(target, rows), :] = values[i * rows : (i + 1) * rows, :]
    saves = []
    for k, span in enumerate(spans):
        loads[3 + k].wait()
        both = jnp.dot(gated[...], weights[:, span], preferred_element_type=f32)
        send[:, span] = both[: 4 * rows]
        keep[:, span] = both[4 * rows :]
        for j, (src, dst) in enumerate(((send, send_hbm), (keep, keep_hbm))):
            saves.append(
                pltpu.make_async_copy(src.at[:, span], dst.at[:, span], sems.at[7 + 2 * k + j])
            )
            saves[-1].start()
    for c in saves:
        c.wait()


def mixer_out_parts(gate, states, decays, carries, out_proj):
    rows, width = gate.shape[0], out_proj.shape[1]
    shape = jax.ShapeDtypeStruct((rows // 2, width), f32)
    return pl.pallas_call(
        mixer_out_kernel,
        out_shape=(shape, shape),
        in_specs=[hbm(), hbm(), hbm(), vmem(), hbm()],
        out_specs=(hbm(), hbm()),
        scratch_shapes=[pltpu.VMEM(gate.shape, f32)] * 3
        + [
            pltpu.VMEM(out_proj.shape, bf16),
            pltpu.VMEM(gate.shape, bf16),
            pltpu.VMEM(shape.shape, f32),
            pltpu.VMEM(shape.shape, f32),
            pltpu.SemaphoreType.DMA((15,)),
        ],
        name="mixer_out",
        **params(58, 3),
    )(gate, states, decays, carries, out_proj)


def combine_kernel(back, slots, weights, shared, out):
    count = slots.shape[1]
    down = lax.broadcasted_iota(jnp.int32, (back.shape[0], count), 0)
    same = lax.broadcasted_iota(jnp.int32, (count, count), 0) == lax.broadcasted_iota(
        jnp.int32, (count, count), 1
    )
    total = shared[...]
    for k in range(2):
        hit = jnp.where(slots[k : k + 1, :] == down, 1.0, 0.0).astype(bf16)
        picked = lax.dot_general(
            hit, back[...], (((0,), (0,)), ((), ())), preferred_element_type=f32
        )
        weight = jnp.sum(jnp.where(same, weights[k : k + 1, :], 0.0), axis=1, keepdims=True)
        total = total + weight * picked
    out[...] = total


def combined(back, slots, weights, shared):
    return pl.pallas_call(
        combine_kernel,
        out_shape=jax.ShapeDtypeStruct(shared.shape, f32),
        in_specs=[vmem()] * 4,
        out_specs=vmem(),
        name="combine",
        **params(12, 3),
    )(back, slots, weights, shared)


def fold_kernel(keep_hbm, other_hbm, own, *refs):
    outs, (keep, other, sems) = refs[:3], refs[3:]
    rows = own.shape[0]
    chip = seat()[1]
    turns = (1, 3, 2, 0)
    loads = []
    for k, s in enumerate(turns):
        take = pl.ds(pl.multiple_of(((chip + s) % 4) * rows, rows), rows)
        pair = [
            pltpu.make_async_copy(src.at[take, :], dst.at[k], sems.at[2 * k + j])
            for j, (src, dst) in enumerate(((keep_hbm, keep), (other_hbm, other)))
        ]
        for c in pair:
            c.start()
        loads.append(pair)
    for k, out in enumerate((*outs, own)):
        for c in loads[k]:
            c.wait()
        out[...] = (keep[k] + other[k]).astype(out.dtype)


def folded(keep, other):
    rows, width = keep.shape[0] // 4, keep.shape[1]
    narrow = jax.ShapeDtypeStruct((rows, width), bf16)
    return pl.pallas_call(
        fold_kernel,
        out_shape=(jax.ShapeDtypeStruct((rows, width), f32), narrow, narrow, narrow),
        in_specs=[hbm(), hbm()],
        out_specs=(vmem(),) * 4,
        scratch_shapes=[
            pltpu.VMEM((4, rows, width), f32),
            pltpu.VMEM((4, rows, width), f32),
            pltpu.SemaphoreType.DMA((8,)),
        ],
        name="fold",
        **params(8, 2),
    )(keep, other)


def mixer_norm_kernel(own, a, b, c, scale, out):
    total = own[...] + a[...].astype(f32) + b[...].astype(f32) + c[...].astype(f32)
    out[...] = normed_block(total, scale[...]).astype(bf16)


def mixer_normed(own, pieces, scale):
    return pl.pallas_call(
        mixer_norm_kernel,
        out_shape=jax.ShapeDtypeStruct(own.shape, bf16),
        in_specs=[vmem()] * 5,
        out_specs=vmem(),
        name="mixer_norm",
        **params(6, 1.5),
    )(own, *pieces, scale)


def expert_norm_kernel(whole, scale, out):
    count, _, _ = whole.shape
    values = jnp.concatenate([whole[j] for j in range(count)], axis=1)
    out[...] = normed_block(values, scale[...]).astype(bf16)


def expert_normed_out(whole, scale):
    count, rows, width = whole.shape
    return pl.pallas_call(
        expert_norm_kernel,
        out_shape=jax.ShapeDtypeStruct((rows, count * width), bf16),
        in_specs=[vmem()] * 2,
        out_specs=vmem(),
        name="expert_norm",
        **params(6, 1.5),
    )(whole, scale)


def swapped(block):
    return lax.ppermute(block, "tp", [(i, i ^ 1) for i in range(8)])


def turned(block, by):
    return lax.ppermute(block, "tp", [(i, (i + 2 * by) % 8) for i in range(8)])


def after(value, *others):
    return lax.optimization_barrier((value, *others))[0]


def gathered(block):
    pieces = [block] + [turned(block, s) for s in (1, 3, 2)]
    return pieces + [swapped(p) for p in pieces]


def whole_body(
    mixer_rows, mixer_gain, gate_proj, input_proj, conv_taps, input_gates, decay_gates,
    decay_offset, out_proj, mixer_scale, expert_rows, expert_gain, route_ids, route_weights,
    expert_gate, expert_up, expert_down, shared_gate, shared_up, shared_down, expert_scale,
):
    rows, width = mixer_rows.shape
    experts = lax.axis_size("ep")
    capacity = rows * 2 * 3 // (2 * experts)
    half = width // 2
    order = (1, 3, 2)

    outgoing, expert_normed, slots, tail = expert_front(
        expert_rows, expert_gain.reshape(1, -1), route_ids.T, mixer_rows, experts, capacity
    )
    halo = lax.ppermute(tail, "ep", [(i, i + 1) for i in range(15)])
    received = lax.all_to_all(
        outgoing.reshape(experts, capacity, half), "ep", 0, 0, tiled=True
    ).reshape(experts * capacity, half)

    hidden_width = expert_gate.shape[2]
    send_rows, *keep_downs, send_downs = prepared(
        expert_gate[0], expert_up[0], after(expert_down[0], slots), shared_down
    )
    shared_hidden = (
        jax.nn.silu(jnp.dot(expert_normed, shared_gate, preferred_element_type=f32))
        * jnp.dot(expert_normed, shared_up, preferred_element_type=f32)
    ).astype(bf16)
    shared_all = gathered(shared_hidden)
    other_rows = swapped(send_rows)
    pair_downs = swapped(send_downs)
    downs = [
        side[s] if s == 0 else turned(side[s], s)
        for side in (keep_downs, pair_downs)
        for s in (0, *order)
    ]

    gate_branch, local_states, decay_product, carry = mixer_local(
        after(mixer_rows, shared_hidden, send_rows), halo, mixer_gain.reshape(1, -1), gate_proj, input_proj,
        conv_taps, input_gates, decay_gates, decay_offset.reshape(1, -1),
    )
    received = after(received, carry)
    own_part, other_part = expert_parts(received, expert_gate[0], expert_up[0], other_rows)
    parts = own_part + swapped(other_part)
    copy_hidden = (jax.nn.silu(parts[:, :hidden_width]) * parts[:, hidden_width:]).astype(bf16)
    hidden_all = gathered(copy_hidden)
    carry = after(carry, copy_hidden)
    carries = lax.all_to_all(
        jnp.broadcast_to(carry[None], (experts, *carry.shape)), "ep", 0, 0, tiled=True
    )
    results = down_projected(hidden_all, downs, 0, bf16)
    shared_term = down_projected(
        [after(shared_all[0], results), *shared_all[1:]], downs, hidden_width, f32
    )
    back = lax.all_to_all(
        results.reshape(experts, capacity, -1), "ep", 0, 0, tiled=True
    ).reshape(experts * capacity, -1)

    carries = after(carries, results)
    keep_term, send_term = mixer_out_parts(
        gate_branch, local_states, decay_product, carries, out_proj
    )
    mixer_own, *mixer_sends = folded(keep_term, swapped(send_term))
    mixer_pieces = [turned(p, s) for p, s in zip(mixer_sends, order)]
    mixer_out = mixer_normed(mixer_own, mixer_pieces, mixer_scale.reshape(1, -1))

    expert_sum = combined(back, slots, route_weights.T, shared_term)
    expert_whole = lax.all_to_all(expert_sum.reshape(8, rows // 8, -1), "tp", 0, 0, tiled=True)
    expert_out = expert_normed_out(expert_whole, expert_scale.reshape(1, -1))
    return (mixer_out, expert_out)


def solution(mesh):
    placed = (
        P("ep", None), P(), P(None, "tp"), P(None, "tp"), P(None, "tp"), P("tp", None, None),
        P("tp", None, None), P("tp"), P("tp", None), P(), P("ep", None), P(), P("ep", None),
        P("ep", None), P("ep", None, "tp"), P("ep", None, "tp"), P("ep", "tp", None),
        P(None, "tp"), P(None, "tp"), P("tp", None), P(),
    )
    return jax.shard_map(
        whole_body,
        mesh=mesh,
        in_specs=placed,
        out_specs=(P(("ep", "tp"), None), P(("ep", "tp"), None)),
        check_vma=False,
    )
```
